32 devices in a mesh: sp: 8 (over z, y), dp: 4 (over x, core).
Axes of the slice: x: 2, y: 2, z: 4, core: 2. Of those that a mesh axis runs over, the one named last changes fastest.
Arguments:
- resid: bfloat16 [4, 2048, 2048], P('dp', 'sp'), may hold values from -6 to 6
- mixer_inputs: bfloat16 [4, 2048, 4096], P('dp', 'sp'), may hold values from -6 to 6
- output_gate: bfloat16 [4, 2048, 4096], P('dp', 'sp'), may hold values from -6 to 6
- write_rows_input: bfloat16 [4, 2048, 256], P('dp', 'sp'), may hold values from -6 to 6
- read_rows_input: bfloat16 [4, 2048, 256], P('dp', 'sp'), may hold values from -6 to 6
- step_size_logits: bfloat16 [4, 2048, 64, 2], P('dp', 'sp'), may hold values from -5 to 5
- extra_log_decay: bfloat16 [4, 2048, 64, 2], P('dp', 'sp'), may hold values from -0.7 to 0
- mixer_conv_taps: bfloat16 [5, 4096], P(None, 'sp'), may hold values from -2.5 to 2.5
- write_conv_taps: bfloat16 [5, 256], replicated, may hold values from -2.5 to 2.5
- read_conv_taps: bfloat16 [5, 256], replicated, may hold values from -2.5 to 2.5
- step_size_bias: float32 [64, 2], P('sp'), may hold values from -20 to -3
- decay_speed: float32 [64, 2], P('sp'), may hold values from 1 to 16
- grouped_norm_gain: float32 [4096], replicated, may hold values from 0.1 to 1.9
- output_matrix: bfloat16 [4096, 2048], P(None, 'dp'), may hold values from -0.09375 to 0.09375
- output_gain: float32 [2048], replicated, may hold values from 0.1 to 1.9
- feedforward_gain: float32 [2048], replicated, may hold values from 0.1 to 1.9
- routes: int32 [4, 2048, 2], P('dp', 'sp'), may hold values from 0 to 7, all different within a row; in each aligned block of 256 rows (0 to 255, 256 to 511, ..., all dimensions but the last counted through in order) at most 96 rows name the same one
- route_weights: float32 [4, 2048, 2], P('dp', 'sp'), may hold values from 0.1 to 1
- expert_gate_weight: bfloat16 [8, 2048, 1024], P('sp'), may hold values from -0.125 to 0.125
- expert_up_weight: bfloat16 [8, 2048, 1024], P('sp'), may hold values from -0.125 to 0.125
- expert_down_weight: bfloat16 [8, 1024, 2048], P('sp'), may hold values from -0.1875 to 0.1875
- expert_sum_gain: float32 [2048], replicated, may hold values from 0.1 to 1.9
Outputs:
- mixed_out: bfloat16 [4, 2048, 2048], P('dp', 'sp')
The draws below stay inside these ranges and needn't reach their ends.
Inputs may be any that keep to these rules, and one draw needn't show every extreme that they name: `routes`: each token names 2 different experts; the 256 positions of one device name one expert at most 96 times, a bound that some block reaches.
All inputs are finite; a program needn't handle non-finite values.
Results may differ from the reference program's by a relative error of at most 0.012.
Values may be sent and summed in bfloat16 or wider, within the bound.
A program may use at most 128 MiB of HBM per device.

```python
import math
import jax
import jax.numpy as jnp
import numpy as np
from jax import lax

D = 2048
HEADS = 64
HEAD_DIM = 64
GROUPS = 2
STATE = 128
CONV_SPAN = 5
BLOCK = 128
FF = 1024
TOPK = 2
TOK_DEV = 256
INNER = 4096
SEQS = 4
SEQ_LEN = 2048
EXPERTS = 8
CAP = 96
N_SP = 8


def decay_pair(key):
    rate_key, pick_key, slow_key, fast_key = jax.random.split(jax.random.fold_in(key, 11), 4)
    rates = jnp.exp(jax.random.uniform(rate_key, (HEADS, 2), jnp.float32, 0.0, math.log(16.0)))
    ranking = jax.random.permutation(pick_key, HEADS * 2).reshape(HEADS, 2)
    quick = ranking < HEADS
    slow_mass = jax.random.uniform(slow_key, (HEADS, 2), jnp.float32, 0.15, 0.45) / SEQ_LEN
    fast_mass = jax.random.uniform(fast_key, (HEADS, 2), jnp.float32, 1.0 / 60.0, 1.0 / 25.0)
    target = jnp.where(quick, fast_mass, slow_mass) / rates
    return (rates, jnp.log(jnp.expm1(target)))


def draw_decay_speed(key, part):
    return decay_pair(key)[0]


def draw_step_size_bias(key, part):
    return decay_pair(key)[1]


def draw_step_size_logits(key, part):
    noise_key, shift_key = jax.random.split(jax.random.fold_in(key, 23))
    shape_full = (SEQS, SEQ_LEN // TOK_DEV, TOK_DEV, HEADS, 2)
    noise = jax.random.normal(noise_key, shape_full, jnp.float32)
    shifts = jax.random.uniform(shift_key, (SEQS, SEQ_LEN // TOK_DEV, 1, HEADS, 2), jnp.float32, -1.5, 1.0)
    shifted = jnp.clip(noise + shifts, -5.0, 5.0)
    return shifted.reshape(SEQS, SEQ_LEN, HEADS, 2).astype(jnp.bfloat16)


def draw_extra_log_decay(key, part):
    hit_key, depth_key = jax.random.split(jax.random.fold_in(key, 31))
    shape_full = (SEQS, SEQ_LEN, HEADS, 2)
    hits = jax.random.uniform(hit_key, shape_full, jnp.float32) < 2.0 / SEQ_LEN
    depth = jax.random.uniform(depth_key, shape_full, jnp.float32, 0.22, 0.69)
    return jnp.where(hits, -depth, 0.0).astype(jnp.bfloat16)


def shard_levels(stream_key, shape, cuts, least, largest):
    def one(position, parts):
        steps = jax.random.uniform(jax.random.fold_in(jax.random.fold_in(stream_key, 6), position), (parts,), jnp.float32, least / len(cuts), largest / len(cuts))
        return jnp.repeat(jnp.exp(steps), shape[position] // parts).reshape((-1,) + (1,) * (len(shape) - position - 1))

    level = one(*cuts[0])
    for cut in cuts[1:]:
        level = level * one(*cut)
    return level


def deal_out(rng, own, number, rows, amount, top, bound, slope):
    order = jax.random.permutation(rng, amount)
    packed, ordinary = portions_of(amount, rows * top, bound, slope, True), portions_of(amount, rows * top, bound, slope, False)
    places = jnp.arange(amount)

    def named(lengths, turn):
        used = int((lengths > 0).sum())
        fixed = max(1, used // 4)
        passed = fixed + (places - fixed + turn * (used - fixed)) % max(1, amount - fixed)
        return jnp.zeros((amount,), jnp.int32).at[order[jnp.where(places < fixed, places, passed)]].set(jnp.asarray(lengths, jnp.int32))

    lengths = jnp.where(number % 4 == 0, named(packed, number // 4), named(ordinary, number - number // 4 - 1))
    mixed = jax.random.permutation(jax.random.fold_in(own, 3), amount)
    source_of, taker = mixed[0:amount // 2 * 2:2], mixed[1:amount // 2 * 2:2]
    room = jnp.minimum(lengths[source_of] - 1, bound - lengths[taker]) // 2
    room = jnp.where((source_of == order[0]) | (taker == order[0]) | (lengths[taker] == 0), 0, jnp.maximum(room, 0))
    passed = jax.random.randint(jax.random.fold_in(own, 4), (amount // 2,), 0, 1 << 20) % (room + 1)
    lengths = lengths.at[source_of].add(-passed).at[taker].add(passed)
    labels = jnp.searchsorted(jnp.cumsum(lengths), jnp.arange(rows * top), side="right").astype(jnp.int32)
    grid = labels.reshape(top, rows).T
    grid = grid[jax.random.permutation(jax.random.fold_in(own, 1), rows)]
    turn = jax.random.randint(jax.random.fold_in(own, 2), (rows, 1), 0, top)
    return jnp.take_along_axis(grid, (jnp.arange(top)[None, :] + turn) % top, axis=1)


def portions_of(amount, total, reach, skew, full):
    weights = [(1 << 20) // math.isqrt(standing ** skew) + 1 for standing in range(1, amount + 1)]
    largest = reach if full else min(reach, max(-(-total // amount), total * weights[0] // sum(weights)))
    least = 1 if total - largest >= amount - 1 else 0
    counts, spare = [largest] + [least] * (amount - 1), total - largest - least * (amount - 1)
    while spare > 0:
        free = [i for i in range(1, amount) if counts[i] < largest] or [i for i in range(1, amount) if counts[i] < reach]
        pool, left = sum([weights[i] for i in free]), spare
        for i in free:
            extra = min(reach - counts[i], max(1, left * weights[i] // pool), spare)
            counts[i] = counts[i] + extra
            spare = spare - extra
    return np.array(counts)


def gaussian(key, shape, scale, most, shards=(), kind=jnp.bfloat16):
    loudness = shard_levels(key, shape, shards, -0.22, 0.18) if shards else 1.0
    entries = jax.random.normal(key, shape, jnp.float32) * scale * loudness
    return jnp.minimum(jnp.maximum(entries, -most), most).astype(kind)


def setup_inputs(seed: int = 0) -> dict:
    key_of = jax.random.split(jax.random.key(seed), 23)
    resid = gaussian(key_of[0], (SEQS, SEQ_LEN, D), 1.0, 6.0, ((0, 4), (1, 8)))
    mixer_inputs = gaussian(key_of[1], (SEQS, SEQ_LEN, INNER), 1.0, 6.0, ((0, 4), (1, 8)))
    output_gate = gaussian(key_of[2], (SEQS, SEQ_LEN, INNER), 1.0, 6.0, ((0, 4), (1, 8)))
    write_rows_input = gaussian(key_of[3], (SEQS, SEQ_LEN, GROUPS * STATE), 1.0, 6.0, ((0, 4), (1, 8)))
    read_rows_input = gaussian(key_of[4], (SEQS, SEQ_LEN, GROUPS * STATE), 1.0, 6.0, ((0, 4), (1, 8)))
    step_size_logits = draw_step_size_logits(jax.random.fold_in(key_of[22], 71), 0)
    extra_log_decay = draw_extra_log_decay(jax.random.fold_in(key_of[22], 71), 0)
    mixer_conv_taps = gaussian(key_of[7], (CONV_SPAN, INNER), CONV_SPAN ** -0.5, 2.5, ((1, 8),))
    write_conv_taps = gaussian(key_of[8], (CONV_SPAN, GROUPS * STATE), CONV_SPAN ** -0.5, 2.5)
    read_conv_taps = gaussian(key_of[9], (CONV_SPAN, GROUPS * STATE), CONV_SPAN ** -0.5, 2.5)
    step_size_bias = draw_step_size_bias(jax.random.fold_in(key_of[22], 71), 0)
    decay_speed = draw_decay_speed(jax.random.fold_in(key_of[22], 71), 0)
    grouped_norm_gain = jnp.clip(1.0 + 0.18 * jax.random.normal(key_of[12], (INNER,), jnp.float32), 0.1, 1.9)
    output_matrix = gaussian(key_of[13], (INNER, D), INNER ** -0.5, 0.09375, ((1, 4),))
    output_gain = jnp.clip(1.0 + 0.18 * jax.random.normal(key_of[14], (D,), jnp.float32), 0.1, 1.9)
    feedforward_gain = jnp.clip(1.0 + 0.18 * jax.random.normal(key_of[15], (D,), jnp.float32), 0.1, 1.9)
    routes_keys = jax.random.split(jax.random.fold_in(key_of[16], 1), SEQS * SEQ_LEN // TOK_DEV)
    routes_turns = jax.random.permutation(jax.random.fold_in(key_of[16], 3), SEQS * SEQ_LEN // TOK_DEV)
    routes = jax.vmap(lambda own, number: deal_out(jax.random.fold_in(key_of[16], 2), own, number, TOK_DEV, EXPERTS, TOPK, CAP, 2))(routes_keys, routes_turns).reshape((SEQS, SEQ_LEN, TOPK))
    route_weights = jnp.clip(jnp.exp(math.log(1.0) - 2.3025851 * jax.random.uniform(key_of[17], (SEQS, SEQ_LEN, TOPK), jnp.float32) ** shard_levels(key_of[17], (SEQS, SEQ_LEN, TOPK), ((0, 4), (1, 8)), -0.2, 0.2)), 0.1, 1.0)
    expert_gate_weight = gaussian(key_of[18], (EXPERTS, D, FF), D ** -0.5, 0.125, ((0, 8),))
    expert_up_weight = gaussian(key_of[19], (EXPERTS, D, FF), D ** -0.5, 0.125, ((0, 8),))
    expert_down_weight = gaussian(key_of[20], (EXPERTS, FF, D), FF ** -0.5, 0.1875, ((0, 8),))
    expert_sum_gain = jnp.clip(1.0 + 0.18 * jax.random.normal(key_of[21], (D,), jnp.float32), 0.1, 1.9)
    return dict(resid=resid, mixer_inputs=mixer_inputs, output_gate=output_gate, write_rows_input=write_rows_input, read_rows_input=read_rows_input, step_size_logits=step_size_logits, extra_log_decay=extra_log_decay, mixer_conv_taps=mixer_conv_taps, write_conv_taps=write_conv_taps, read_conv_taps=read_conv_taps, step_size_bias=step_size_bias, decay_speed=decay_speed, grouped_norm_gain=grouped_norm_gain, output_matrix=output_matrix, output_gain=output_gain, feedforward_gain=feedforward_gain, routes=routes, route_weights=route_weights, expert_gate_weight=expert_gate_weight, expert_up_weight=expert_up_weight, expert_down_weight=expert_down_weight, expert_sum_gain=expert_sum_gain)


EPS = 1e-06

def rms_scale(values, scale_gain):
    return values * lax.rsqrt(lax.optimization_barrier(jnp.mean(values * values, axis=-1, keepdims=True)) + EPS) * scale_gain

def rounded(values):
    return lax.optimization_barrier(values.astype(jnp.bfloat16)).astype(jnp.float32)

def centred_conv(values, kernel):
    span_len = kernel.shape[0]
    half_span = span_len // 2
    length = values.shape[0]
    padded = jnp.pad(values.astype(jnp.float32), ((half_span, half_span), (0, 0)))
    summed = jnp.zeros(values.shape, jnp.float32)
    for offset in range(span_len):
        summed = summed + padded[offset:offset + length] * kernel[offset].astype(jnp.float32)
    return jax.nn.silu(summed).astype(jnp.bfloat16)

def block_pass(inputs, writes, read_rows, head_step_sizes, logarithm_decay):
    length = inputs.shape[0]
    blocks = length // BLOCK
    inp_block = inputs.reshape(blocks, BLOCK, -1).astype(jnp.float32)
    wr_block = writes.reshape(blocks, BLOCK, -1).astype(jnp.float32)
    rd_block = read_rows.reshape(blocks, BLOCK, -1).astype(jnp.float32)
    step_blk = head_step_sizes.reshape(blocks, BLOCK)
    cumulative = jnp.cumsum(logarithm_decay.reshape(blocks, BLOCK), axis=1)
    lower_tri = jnp.tril(jnp.ones((BLOCK, BLOCK), dtype=bool))
    spread = cumulative[:, :, None] - cumulative[:, None, :]
    in_block = jnp.where(lower_tri, jnp.exp(jnp.where(lower_tri, spread, 0.0)), 0.0)
    scores = jnp.einsum('cln,csn->cls', rd_block, wr_block)
    weights = rounded(scores * in_block * step_blk[:, None, :])
    within = jnp.einsum('cls,csp->clp', weights, inp_block)
    to_end = jnp.exp(cumulative[:, -1:] - cumulative) * step_blk
    scaled = rounded(wr_block * to_end[:, :, None])
    states = jnp.einsum('csn,csp->cnp', scaled, inp_block)
    totals = cumulative[:, -1]
    through = jnp.cumsum(totals)
    preceding = through - totals
    strict = jnp.tril(jnp.ones((blocks, blocks), dtype=bool), -1)
    carry_mat = jnp.where(strict, jnp.exp(jnp.where(strict, preceding[:, None] - through[None, :], 0.0)), 0.0)
    entering = jnp.dot(carry_mat, states.reshape(blocks, -1), precision=lax.Precision.HIGHEST)
    entering = rounded(entering.reshape(states.shape))
    carried = jnp.einsum('cln,cnp->clp', rd_block, entering) * jnp.exp(cumulative)[:, :, None]
    return (within + carried).reshape(length, -1)

def both_ways(inputs, writes, read_rows, head_step_sizes, logarithm_decay):
    forward = block_pass(inputs, writes, read_rows, head_step_sizes[:, 0], logarithm_decay[:, 0])
    backward = block_pass(jnp.flip(inputs, 0), jnp.flip(writes, 0), jnp.flip(read_rows, 0), jnp.flip(head_step_sizes[:, 1], 0), jnp.flip(logarithm_decay[:, 1], 0))
    return forward + jnp.flip(backward, 0)

def reference(resid, mixer_inputs, output_gate, write_rows_input, read_rows_input, step_size_logits, extra_log_decay, mixer_conv_taps, write_conv_taps, read_conv_taps, step_size_bias, decay_speed, grouped_norm_gain, output_matrix, output_gain, feedforward_gain, routes, route_weights, expert_gate_weight, expert_up_weight, expert_down_weight, expert_sum_gain):
    per_group = HEADS // GROUPS

    def single_sequence(packed_values):
        sequence_inputs, sequence_write_rows, sequence_read_rows, sequence_step_pre, sequence_extra_decay = packed_values
        length = sequence_inputs.shape[0]
        x_act = centred_conv(sequence_inputs, mixer_conv_taps).reshape(length, HEADS, HEAD_DIM)
        write_act = jnp.repeat(centred_conv(sequence_write_rows, write_conv_taps).reshape(length, GROUPS, STATE), per_group, axis=1)
        read_act = jnp.repeat(centred_conv(sequence_read_rows, read_conv_taps).reshape(length, GROUPS, STATE), per_group, axis=1)
        head_step_sizes = jax.nn.softplus(sequence_step_pre.astype(jnp.float32) + step_size_bias)
        logarithm_decay = sequence_extra_decay.astype(jnp.float32) - decay_speed * head_step_sizes

        def one_head(packed_head):
            return both_ways(*packed_head).astype(jnp.bfloat16)
        moved = tuple((jnp.moveaxis(item, 1, 0) for item in (x_act, write_act, read_act, head_step_sizes, logarithm_decay)))
        return jnp.moveaxis(lax.map(one_head, moved), 0, 1)
    head_outputs = lax.map(single_sequence, (mixer_inputs, write_rows_input, read_rows_input, step_size_logits, extra_log_decay))
    tokens = SEQS * SEQ_LEN
    gated_vals = head_outputs.reshape(tokens, INNER).astype(jnp.float32) * jax.nn.silu(output_gate.reshape(tokens, INNER).astype(jnp.float32))
    grouped = gated_vals.reshape(tokens, GROUPS, INNER // GROUPS)
    grouped = grouped * lax.rsqrt(lax.optimization_barrier(jnp.mean(grouped * grouped, axis=-1, keepdims=True)) + EPS)
    normed = (grouped.reshape(tokens, INNER) * grouped_norm_gain).astype(jnp.bfloat16)
    projected = jnp.dot(normed, output_matrix, preferred_element_type=jnp.float32)
    resid_one = (resid.reshape(tokens, D).astype(jnp.float32) + rms_scale(projected, output_gain)).astype(jnp.bfloat16)
    ffn_in = rms_scale(resid_one.astype(jnp.float32), feedforward_gain).astype(jnp.bfloat16)
    padded_in = jnp.concatenate([ffn_in, jnp.zeros((1, D), jnp.bfloat16)], axis=0)
    flat_route = routes.reshape(-1)
    flat_weight = jnp.concatenate([route_weights.reshape(-1), jnp.zeros((1,), jnp.float32)], axis=0)
    assign_count = tokens * TOPK
    slot_count = SEQS * N_SP * CAP

    def one_expert(combined, expert):
        slot_index = jnp.nonzero(flat_route == expert, size=slot_count, fill_value=assign_count)[0].astype(jnp.int32)
        token_index = slot_index // TOPK
        picked_rows = padded_in[token_index]
        gate_part = jnp.dot(picked_rows, expert_gate_weight[expert], preferred_element_type=jnp.float32)
        up_part = jnp.dot(picked_rows, expert_up_weight[expert], preferred_element_type=jnp.float32)
        hidden = (jax.nn.silu(gate_part) * up_part).astype(jnp.bfloat16)
        result = jnp.dot(hidden, expert_down_weight[expert], preferred_element_type=jnp.float32).astype(jnp.bfloat16)
        combined = combined.at[token_index].add(result.astype(jnp.float32) * flat_weight[slot_index][:, None])
        return (combined, None)
    combined, _ = lax.scan(one_expert, jnp.zeros((tokens + 1, D), jnp.float32), jnp.arange(EXPERTS, dtype=jnp.int32))
    mixed_out = resid_one.astype(jnp.float32) + rms_scale(combined[:tokens], expert_sum_gain)
    return mixed_out.astype(jnp.bfloat16).reshape(SEQS, SEQ_LEN, D)
```

```python
import functools

import jax
import jax.numpy as jnp
from jax import lax
from jax.experimental import pallas as pl
from jax.experimental.pallas import tpu as pltpu
from jax.sharding import PartitionSpec as P

D = 2048
HEADS = 64
HEAD_DIM = 64
GROUPS = 2
STATE = 128
BLOCK = 128
TOPK = 2
INNER = 4096
PAD = 16


EPS = 1e-06


def rms_scale(values, scale_gain):
    return values * lax.rsqrt(jnp.mean(values * values, axis=-1, keepdims=True) + EPS) * scale_gain


def silu(values):
    return values / (1.0 + jnp.exp(-values))


def spread_pair(first, second, low_half):
    wide = (first.shape[0], BLOCK)
    return jnp.where(low_half, jnp.broadcast_to(first, wide), jnp.broadcast_to(second, wide))


def mixer_kernel(
    local_heads, x_ref, w_ref, r_ref, taps_ref, step_ref, decay_ref, step_t_ref, decay_t_ref,
    out_ref, padded, act, partial_y, cumul, state,
):
    length = out_ref.shape[0]
    width = out_ref.shape[1]
    blocks = length // BLOCK
    half = taps_ref.shape[0] // 2
    cols = width + 2 * STATE
    padded[0:PAD, :] = jnp.zeros((PAD, cols), jnp.bfloat16)
    padded[PAD + length : 2 * PAD + length, :] = jnp.zeros((PAD, cols), jnp.bfloat16)
    padded[PAD : PAD + length, 0:width] = x_ref[:, 0:width]
    padded[PAD : PAD + length, width : width + STATE] = w_ref[...]
    padded[PAD : PAD + length, width + STATE : cols] = r_ref[...]
    row_id = lax.broadcasted_iota(jnp.int32, (BLOCK, BLOCK), 0)
    col_id = lax.broadcasted_iota(jnp.int32, (BLOCK, BLOCK), 1)
    lower = row_id >= col_id
    diagonal = row_id == col_id
    tri = lower.astype(jnp.float32)
    tri_t = (row_id <= col_id).astype(jnp.float32)
    low_half = col_id < HEAD_DIM
    high = lax.Precision.HIGHEST

    state[...] = jnp.zeros_like(state)

    def forward(block, carry):
        start = pl.multiple_of(block * BLOCK, BLOCK)
        rows = pl.ds(start, BLOCK)
        for lo in range(0, cols, STATE):
            piece = padded[pl.ds(start, BLOCK + 2 * PAD), lo : lo + STATE].astype(jnp.float32)
            summed = jnp.zeros((BLOCK, STATE), jnp.float32)
            for offset in range(2 * half + 1):
                at = PAD - half + offset
                summed = summed + piece[at : at + BLOCK] * taps_ref[offset : offset + 1, lo : lo + STATE]
            act[rows, lo : lo + STATE] = silu(summed).astype(jnp.bfloat16)
        write = act[rows, width : width + STATE]
        read = act[rows, width + STATE : cols]
        decay = decay_ref[rows, :]
        cum = jnp.dot(tri, decay, precision=high, preferred_element_type=jnp.float32)
        cum_t = jnp.dot(
            decay_t_ref[:, rows], tri_t, precision=high, preferred_element_type=jnp.float32
        )
        before = cum - decay
        cumul[rows, :] = before
        before_t = cum_t - decay_t_ref[:, rows]
        step = step_ref[rows, :]
        step_t = step_t_ref[:, rows]
        scores = lax.dot_general(
            read, write, (((1,), (1,)), ((), ())), preferred_element_type=jnp.float32
        )
        entering = state[...].astype(jnp.bfloat16)
        carried = jnp.dot(read, entering, preferred_element_type=jnp.float32)
        scaled_parts = []
        leave_parts = []
        for pair in range(local_heads // 2):
            span = slice(pair * BLOCK, (pair + 1) * BLOCK)
            x_pair = act[rows, span]
            weights = []
            for h in (2 * pair, 2 * pair + 1):
                b = local_heads + h
                to_row = jnp.where(lower, cum[:, h : h + 1], -before[:, b : b + 1])
                from_col = jnp.where(lower, cum_t[h : h + 1, :], -before_t[b : b + 1, :])
                mult = jnp.where(lower, step_t[h : h + 1, :], step_t[b : b + 1, :])
                mult = mult + jnp.where(diagonal, step_t[b : b + 1, :], 0.0)
                weights.append(
                    (scores * jnp.exp(jnp.minimum(to_row - from_col, 0.0)) * mult).astype(jnp.bfloat16)
                )
            zero = jnp.zeros_like(x_pair)
            stacked = jnp.concatenate(
                [jnp.where(low_half, x_pair, zero), jnp.where(low_half, zero, x_pair)], axis=0
            )
            within = jnp.dot(
                jnp.concatenate(weights, axis=1), stacked, preferred_element_type=jnp.float32
            )
            h = 2 * pair
            cum_pair = spread_pair(cum[:, h : h + 1], cum[:, h + 1 : h + 2], low_half)
            step_pair = spread_pair(step[:, h : h + 1], step[:, h + 1 : h + 2], low_half)
            partial_y[rows, span] = within + carried[:, span] * jnp.exp(cum_pair)
            total = cum_pair[BLOCK - 1 : BLOCK, :]
            to_end = jnp.exp(total - cum_pair) * step_pair
            scaled_parts.append((x_pair.astype(jnp.float32) * to_end).astype(jnp.bfloat16))
            leave_parts.append(jnp.exp(total))
        scaled = jnp.concatenate(scaled_parts, axis=1)
        leaving = jnp.concatenate(leave_parts, axis=1)
        state[...] = state[...] * leaving + lax.dot_general(
            write, scaled, (((0,), (0,)), ((), ())), preferred_element_type=jnp.float32
        )
        return carry

    lax.fori_loop(0, blocks, forward, 0)
    state[...] = jnp.zeros_like(state)

    def backward(back, carry):
        block = blocks - 1 - back
        rows = pl.ds(pl.multiple_of(block * BLOCK, BLOCK), BLOCK)
        write = act[rows, width : width + STATE]
        read = act[rows, width + STATE : cols]
        before = cumul[rows, :]
        decay = decay_ref[rows, :]
        step = step_ref[rows, :]
        entering = state[...].astype(jnp.bfloat16)
        carried = jnp.dot(read, entering, preferred_element_type=jnp.float32)
        scaled_parts = []
        leave_parts = []
        for pair in range(local_heads // 2):
            span = slice(pair * BLOCK, (pair + 1) * BLOCK)
            x_pair = act[rows, span]
            b = local_heads + 2 * pair
            before_pair = spread_pair(before[:, b : b + 1], before[:, b + 1 : b + 2], low_half)
            step_pair = spread_pair(step[:, b : b + 1], step[:, b + 1 : b + 2], low_half)
            last = BLOCK - 1
            total = before_pair[last : last + 1, :] + spread_pair(
                decay[last : last + 1, b : b + 1],
                decay[last : last + 1, b + 1 : b + 2],
                low_half[0:1, :],
            )
            out_ref[rows, span] = (
                partial_y[rows, span] + carried[:, span] * jnp.exp(total - before_pair)
            ).astype(jnp.bfloat16)
            to_start = jnp.exp(before_pair) * step_pair
            scaled_parts.append((x_pair.astype(jnp.float32) * to_start).astype(jnp.bfloat16))
            leave_parts.append(jnp.exp(total))
        scaled = jnp.concatenate(scaled_parts, axis=1)
        leaving = jnp.concatenate(leave_parts, axis=1)
        state[...] = state[...] * leaving + lax.dot_general(
            write, scaled, (((0,), (0,)), ((), ())), preferred_element_type=jnp.float32
        )
        return carry

    lax.fori_loop(0, blocks, backward, 0)


def run_mixer(local_heads, x, write, read, taps, step, decay):
    length = x.shape[0]
    width = local_heads * HEAD_DIM
    cols = width + 2 * STATE
    vmem = pl.BlockSpec(memory_space=pltpu.VMEM)
    return pl.pallas_call(
        functools.partial(mixer_kernel, local_heads),
        out_shape=jax.ShapeDtypeStruct((length, width), jnp.bfloat16),
        in_specs=[vmem] * 8,
        out_specs=vmem,
        scratch_shapes=[
            pltpu.VMEM((length + 2 * PAD, cols), jnp.bfloat16),
            pltpu.VMEM((length, cols), jnp.bfloat16),
            pltpu.VMEM((length, width), jnp.float32),
            pltpu.VMEM((length, 2 * local_heads), jnp.float32),
            pltpu.VMEM((STATE, width), jnp.float32),
        ],
        compiler_params=pltpu.CompilerParams(vmem_limit_bytes=56 * 1024 * 1024),
        cost_estimate=pl.CostEstimate(
            flops=20 * length * width * BLOCK, bytes_accessed=8 * length * width, transcendentals=0
        ),
        name="mixer",
    )(x, write, read, taps, step, decay, step.T, decay.T)


def project_kernel(
    heads_ref, gate_ref, norm_gain_ref, matrix_ref, resid_ref, out_gain_ref, ffn_gain_ref,
    resid_one_ref, ffn_in_ref, normed, projected,
):
    step = pl.program_id(0)
    chunks, tok_rows, width = heads_ref.shape
    per_group = chunks // GROUPS

    @pl.when(step == 0)
    def _():
        for group in range(GROUPS):
            total = jnp.zeros((tok_rows, 1), jnp.float32)
            for i in range(group * per_group, (group + 1) * per_group):
                cols = slice(i * width, (i + 1) * width)
                u = heads_ref[i].astype(jnp.float32) * silu(gate_ref[:, cols].astype(jnp.float32))
                total = total + jnp.sum(u * u, axis=1, keepdims=True)
            scale = lax.rsqrt(total * (1.0 / (per_group * width)) + EPS)
            for i in range(group * per_group, (group + 1) * per_group):
                cols = slice(i * width, (i + 1) * width)
                u = heads_ref[i].astype(jnp.float32) * silu(gate_ref[:, cols].astype(jnp.float32))
                normed[:, cols] = (u * scale * norm_gain_ref[:, cols]).astype(jnp.bfloat16)

    parts, _, part = projected.shape
    projected[step] = jnp.dot(normed[...], matrix_ref[0], preferred_element_type=jnp.float32)

    @pl.when(step == pl.num_programs(0) - 1)
    def _():
        total = jnp.zeros((tok_rows, 1), jnp.float32)
        for j in range(parts):
            total = total + jnp.sum(projected[j] * projected[j], axis=1, keepdims=True)
        scale = lax.rsqrt(total * (1.0 / (parts * part)) + EPS)
        total = jnp.zeros((tok_rows, 1), jnp.float32)
        for j in range(parts):
            cols = slice(j * part, (j + 1) * part)
            one = (
                resid_ref[:, cols].astype(jnp.float32) + projected[j] * scale * out_gain_ref[:, cols]
            ).astype(jnp.bfloat16)
            resid_one_ref[:, cols] = one
            one = one.astype(jnp.float32)
            total = total + jnp.sum(one * one, axis=1, keepdims=True)
        scale = lax.rsqrt(total * (1.0 / (parts * part)) + EPS)
        for j in range(parts):
            cols = slice(j * part, (j + 1) * part)
            ffn_in_ref[:, cols] = (
                resid_one_ref[:, cols].astype(jnp.float32) * scale * ffn_gain_ref[:, cols]
            ).astype(jnp.bfloat16)


def run_project(heads, gate, norm_gain, matrix, resid, out_gain, ffn_gain):
    chunks, tok_rows, width = heads.shape
    parts, inner, part = matrix.shape
    model = parts * part

    def whole(shape):
        return pl.BlockSpec(shape, lambda j: (0,) * len(shape))

    return pl.pallas_call(
        project_kernel,
        grid=(parts,),
        out_shape=(
            jax.ShapeDtypeStruct((tok_rows, model), jnp.bfloat16),
            jax.ShapeDtypeStruct((tok_rows, model), jnp.bfloat16),
        ),
        in_specs=[
            whole(heads.shape),
            whole(gate.shape),
            whole((1, inner)),
            pl.BlockSpec((1, inner, part), lambda j: (j, 0, 0)),
            whole(resid.shape),
            whole((1, model)),
            whole((1, model)),
        ],
        out_specs=(whole((tok_rows, model)), whole((tok_rows, model))),
        scratch_shapes=[
            pltpu.VMEM((tok_rows, inner), jnp.bfloat16),
            pltpu.VMEM((parts, tok_rows, part), jnp.float32),
        ],
        compiler_params=pltpu.CompilerParams(vmem_limit_bytes=50 * 1024 * 1024),
        cost_estimate=pl.CostEstimate(
            flops=2 * tok_rows * inner * model, bytes_accessed=2 * inner * model, transcendentals=0
        ),
        name="project",
    )(heads, gate, norm_gain[None], matrix, resid, out_gain[None], ffn_gain[None])


def local(
    resid,
    mixer_inputs,
    output_gate,
    write_rows_input,
    read_rows_input,
    step_size_logits,
    extra_log_decay,
    mixer_conv_taps,
    write_conv_taps,
    read_conv_taps,
    step_size_bias,
    decay_speed,
    grouped_norm_gain,
    output_matrix,
    output_gain,
    feedforward_gain,
    routes,
    route_weights,
    expert_gate_weight,
    expert_up_weight,
    expert_down_weight,
    expert_sum_gain,
):
    tok_rows = mixer_inputs.shape[1]
    local_heads = step_size_bias.shape[0]
    per_group = HEADS // GROUPS
    width = local_heads * HEAD_DIM
    sp_size = lax.axis_size("sp")
    my_sp = lax.axis_index("sp")
    group_id = my_sp * local_heads // per_group
    gathered_rows = lax.all_gather(
        jnp.concatenate([write_rows_input[0], read_rows_input[0]], axis=1), "sp", axis=0, tiled=True
    )
    matrix_now, gathered_rows = lax.optimization_barrier((output_matrix, gathered_rows))
    matrix = lax.all_gather(matrix_now, "dp", axis=0, tiled=False)

    def by_dest(item):
        return jnp.moveaxis(item.reshape(tok_rows, sp_size, -1), 1, 0)

    def split_dirs(item):
        return jnp.moveaxis(
            item.reshape(tok_rows, sp_size, local_heads, 2), (1, 3), (0, 2)
        ).reshape(sp_size, tok_rows, 2 * local_heads)

    route_cols = jnp.broadcast_to(
        routes[0].astype(jnp.bfloat16)[None], (sp_size, tok_rows, TOPK)
    )
    sent = jnp.concatenate(
        [by_dest(mixer_inputs[0]), split_dirs(step_size_logits[0]), split_dirs(extra_log_decay[0]), route_cols],
        axis=2,
    )
    received = lax.all_to_all(sent, "sp", split_axis=0, concat_axis=0, tiled=True)
    received = received.reshape(sp_size * tok_rows, -1)
    dirs = 2 * local_heads
    step_pre = received[:, width : width + dirs].astype(jnp.float32)
    extra = received[:, width + dirs : width + 2 * dirs].astype(jnp.float32)
    routes_all = received[:, width + 2 * dirs :].astype(jnp.int32).reshape(sp_size, tok_rows, TOPK)
    step = jax.nn.softplus(step_pre + step_size_bias.T.reshape(1, dirs))
    decay = extra - decay_speed.T.reshape(1, dirs) * step
    col_start = group_id * STATE
    group_cols = GROUPS * STATE
    write_rows = lax.dynamic_slice_in_dim(gathered_rows, col_start, STATE, 1)
    read_rows = lax.dynamic_slice_in_dim(gathered_rows, group_cols + col_start, STATE, 1)
    taps = jnp.concatenate(
        [
            mixer_conv_taps,
            lax.dynamic_slice_in_dim(write_conv_taps, col_start, STATE, 1),
            lax.dynamic_slice_in_dim(read_conv_taps, col_start, STATE, 1),
        ],
        axis=1,
    ).astype(jnp.float32)
    head_outputs = run_mixer(local_heads, received, write_rows, read_rows, taps, step, decay)
    token_heads = lax.all_to_all(
        head_outputs.reshape(sp_size, tok_rows, width), "sp", split_axis=0, concat_axis=0, tiled=True
    )
    resid_one, ffn_in = run_project(
        token_heads, output_gate[0], grouped_norm_gain, matrix, resid[0], output_gain, feedforward_gain
    )
    local_experts = expert_gate_weight.shape[0]
    experts = local_experts * sp_size
    capacity = 3 * tok_rows * TOPK // (2 * experts)
    my_experts = my_sp * local_experts + jnp.arange(local_experts, dtype=jnp.int32)
    named = jnp.any(
        routes_all[:, None, :, :] == my_experts[None, :, None, None], axis=3
    ).astype(jnp.int32)
    place = jnp.where(named > 0, jnp.cumsum(named, axis=2) - 1, -1)
    slots = jnp.arange(capacity, dtype=jnp.int32)
    tokens = jnp.arange(tok_rows, dtype=jnp.int32)
    slot_token = jnp.sum(
        jnp.where(place[:, :, None, :] == slots[None, None, :, None], tokens, 0), axis=3
    )
    slot_row = slot_token + (jnp.arange(sp_size, dtype=jnp.int32) * tok_rows)[:, None, None]
    my_routes = routes[0]
    one_hot = (my_routes[:, :, None] == jnp.arange(experts, dtype=jnp.int32)).astype(jnp.int32)
    per_token = jnp.sum(one_hot, axis=1)
    earlier = jnp.cumsum(per_token, axis=0) - per_token
    slot_dest = my_routes * capacity + jnp.sum(earlier[:, None, :] * one_hot, axis=2)
    all_tokens = lax.all_gather(ffn_in, "sp", axis=0, tiled=True)
    arrived = all_tokens[slot_row.reshape(-1)].reshape(sp_size, local_experts, capacity, D)
    gate_part = jnp.einsum(
        "sekd,edh->sekh", arrived, expert_gate_weight, preferred_element_type=jnp.float32
    )
    up_part = jnp.einsum(
        "sekd,edh->sekh", arrived, expert_up_weight, preferred_element_type=jnp.float32
    )
    hidden = (jax.nn.silu(gate_part) * up_part).astype(jnp.bfloat16)
    expert_rows = jnp.einsum(
        "sekh,ehd->sekd", hidden, expert_down_weight, preferred_element_type=jnp.float32
    ).astype(jnp.bfloat16)
    returned = lax.all_to_all(expert_rows, "sp", split_axis=0, concat_axis=0, tiled=True)
    returned = returned.reshape(experts * capacity, D)
    combined = sum(
        returned[slot_dest[:, k]].astype(jnp.float32) * route_weights[0][:, k : k + 1]
        for k in range(TOPK)
    )
    mixed_out = resid_one.astype(jnp.float32) + rms_scale(combined, expert_sum_gain)
    return mixed_out.astype(jnp.bfloat16)[None]


def solution(mesh):
    in_specs = (
        P("dp", "sp", None),
        P("dp", "sp", None),
        P("dp", "sp", None),
        P("dp", "sp", None),
        P("dp", "sp", None),
        P("dp", "sp", None, None),
        P("dp", "sp", None, None),
        P(None, "sp"),
        P(),
        P(),
        P("sp", None),
        P("sp", None),
        P(),
        P(None, "dp"),
        P(),
        P(),
        P("dp", "sp", None),
        P("dp", "sp", None),
        P("sp", None, None),
        P("sp", None, None),
        P("sp", None, None),
        P(),
    )
    out_specs = P("dp", "sp", None)
    return jax.shard_map(local, mesh=mesh, in_specs=in_specs, out_specs=out_specs, check_vma=False)
```

```python
import functools

import jax
import jax.numpy as jnp
from jax import lax
from jax.experimental import pallas as pl
from jax.experimental.pallas import tpu as pltpu
from jax.sharding import PartitionSpec as P


D = 2048
HEADS = 64
HEAD_DIM = 64
GROUPS = 2
STATE = 128
BLOCK = 128
TOPK = 2
PAD = 16


EPS = 1e-06


def rms_scale(values, scale_gain):
    return values * lax.rsqrt(jnp.mean(values * values, axis=-1, keepdims=True) + EPS) * scale_gain


def silu(values):
    return values / (1.0 + jnp.exp(-values))


def spread_pair(first, second, low_half):
    wide = (first.shape[0], BLOCK)
    return jnp.where(low_half, jnp.broadcast_to(first, wide), jnp.broadcast_to(second, wide))


def mixer_kernel(
    local_heads, x_ref, rows_ref, taps_ref, step_ref, decay_ref, step_t_ref, decay_t_ref,
    out_ref, padded, act, partial_y, cumul, state,
):
    length = out_ref.shape[0]
    width = out_ref.shape[1]
    blocks = length // BLOCK
    half = taps_ref.shape[0] // 2
    cols = width + 2 * STATE
    padded[0:PAD, :] = jnp.zeros((PAD, cols), jnp.bfloat16)
    padded[PAD + length : 2 * PAD + length, :] = jnp.zeros((PAD, cols), jnp.bfloat16)
    padded[PAD : PAD + length, 0:width] = x_ref[:, 0:width]
    padded[PAD : PAD + length, width:cols] = rows_ref[:, width:cols]
    row_id = lax.broadcasted_iota(jnp.int32, (BLOCK, BLOCK), 0)
    col_id = lax.broadcasted_iota(jnp.int32, (BLOCK, BLOCK), 1)
    lower = row_id >= col_id
    diagonal = row_id == col_id
    tri = lower.astype(jnp.float32)
    tri_t = (row_id <= col_id).astype(jnp.float32)
    low_half = col_id < HEAD_DIM
    high = lax.Precision.HIGHEST

    state[...] = jnp.zeros_like(state)

    def forward(block, carry):
        start = pl.multiple_of(block * BLOCK, BLOCK)
        rows = pl.ds(start, BLOCK)
        for lo in range(0, cols, STATE):
            piece = padded[pl.ds(start, BLOCK + 2 * PAD), lo : lo + STATE].astype(jnp.float32)
            summed = jnp.zeros((BLOCK, STATE), jnp.float32)
            for offset in range(2 * half + 1):
                at = PAD - half + offset
                summed = summed + piece[at : at + BLOCK] * taps_ref[offset : offset + 1, lo : lo + STATE]
            act[rows, lo : lo + STATE] = silu(summed).astype(jnp.bfloat16)
        write = act[rows, width : width + STATE]
        read = act[rows, width + STATE : cols]
        decay = decay_ref[rows, :]
        cum = jnp.dot(tri, decay, precision=high, preferred_element_type=jnp.float32)
        cum_t = jnp.dot(
            decay_t_ref[:, rows], tri_t, precision=high, preferred_element_type=jnp.float32
        )
        before = cum - decay
        cumul[rows, :] = before
        before_t = cum_t - decay_t_ref[:, rows]
        step = step_ref[rows, :]
        step_t = step_t_ref[:, rows]
        scores = lax.dot_general(
            read, write, (((1,), (1,)), ((), ())), preferred_element_type=jnp.float32
        )
        entering = state[...].astype(jnp.bfloat16)
        carried = jnp.dot(read, entering, preferred_element_type=jnp.float32)
        scaled_parts = []
        leave_parts = []
        for pair in range(local_heads // 2):
            span = slice(pair * BLOCK, (pair + 1) * BLOCK)
            x_pair = act[rows, span]
            weights = []
            for h in (2 * pair, 2 * pair + 1):
                b = local_heads + h
                to_row = jnp.where(lower, cum[:, h : h + 1], -before[:, b : b + 1])
                from_col = jnp.where(lower, cum_t[h : h + 1, :], -before_t[b : b + 1, :])
                mult = jnp.where(lower, step_t[h : h + 1, :], step_t[b : b + 1, :])
                mult = mult + jnp.where(diagonal, step_t[b : b + 1, :], 0.0)
                weights.append(
                    (scores * jnp.exp(jnp.minimum(to_row - from_col, 0.0)) * mult).astype(jnp.bfloat16)
                )
            zero = jnp.zeros_like(x_pair)
            stacked = jnp.concatenate(
                [jnp.where(low_half, x_pair, zero), jnp.where(low_half, zero, x_pair)], axis=0
            )
            within = jnp.dot(
                jnp.concatenate(weights, axis=1), stacked, preferred_element_type=jnp.float32
            )
            h = 2 * pair
            cum_pair = spread_pair(cum[:, h : h + 1], cum[:, h + 1 : h + 2], low_half)
            step_pair = spread_pair(step[:, h : h + 1], step[:, h + 1 : h + 2], low_half)
            partial_y[rows, span] = within + carried[:, span] * jnp.exp(cum_pair)
            total = cum_pair[BLOCK - 1 : BLOCK, :]
            to_end = jnp.exp(total - cum_pair) * step_pair
            scaled_parts.append((x_pair.astype(jnp.float32) * to_end).astype(jnp.bfloat16))
            leave_parts.append(jnp.exp(total))
        scaled = jnp.concatenate(scaled_parts, axis=1)
        leaving = jnp.concatenate(leave_parts, axis=1)
        state[...] = state[...] * leaving + lax.dot_general(
            write, scaled, (((0,), (0,)), ((), ())), preferred_element_type=jnp.float32
        )
        return carry

    lax.fori_loop(0, blocks, forward, 0)
    state[...] = jnp.zeros_like(state)

    def backward(back, carry):
        block = blocks - 1 - back
        rows = pl.ds(pl.multiple_of(block * BLOCK, BLOCK), BLOCK)
        write = act[rows, width : width + STATE]
        read = act[rows, width + STATE : cols]
        before = cumul[rows, :]
        decay = decay_ref[rows, :]
        step = step_ref[rows, :]
        entering = state[...].astype(jnp.bfloat16)
        carried = jnp.dot(read, entering, preferred_element_type=jnp.float32)
        scaled_parts = []
        leave_parts = []
        for pair in range(local_heads // 2):
            span = slice(pair * BLOCK, (pair + 1) * BLOCK)
            x_pair = act[rows, span]
            b = local_heads + 2 * pair
            before_pair = spread_pair(before[:, b : b + 1], before[:, b + 1 : b + 2], low_half)
            step_pair = spread_pair(step[:, b : b + 1], step[:, b + 1 : b + 2], low_half)
            last = BLOCK - 1
            total = before_pair[last : last + 1, :] + spread_pair(
                decay[last : last + 1, b : b + 1],
                decay[last : last + 1, b + 1 : b + 2],
                low_half[0:1, :],
            )
            out_ref[rows, span] = (
                partial_y[rows, span] + carried[:, span] * jnp.exp(total - before_pair)
            ).astype(jnp.bfloat16)
            to_start = jnp.exp(before_pair) * step_pair
            scaled_parts.append((x_pair.astype(jnp.float32) * to_start).astype(jnp.bfloat16))
            leave_parts.append(jnp.exp(total))
        scaled = jnp.concatenate(scaled_parts, axis=1)
        leaving = jnp.concatenate(leave_parts, axis=1)
        state[...] = state[...] * leaving + lax.dot_general(
            write, scaled, (((0,), (0,)), ((), ())), preferred_element_type=jnp.float32
        )
        return carry

    lax.fori_loop(0, blocks, backward, 0)


def run_mixer(local_heads, x, rows, taps, step, decay):
    length = x.shape[0]
    width = local_heads * HEAD_DIM
    cols = width + 2 * STATE
    vmem = pl.BlockSpec(memory_space=pltpu.VMEM)
    return pl.pallas_call(
        functools.partial(mixer_kernel, local_heads),
        out_shape=jax.ShapeDtypeStruct((length, width), jnp.bfloat16),
        in_specs=[vmem] * 7,
        out_specs=vmem,
        scratch_shapes=[
            pltpu.VMEM((length + 2 * PAD, cols), jnp.bfloat16),
            pltpu.VMEM((length, cols), jnp.bfloat16),
            pltpu.VMEM((length, width), jnp.float32),
            pltpu.VMEM((length, 2 * local_heads), jnp.float32),
            pltpu.VMEM((STATE, width), jnp.float32),
        ],
        compiler_params=pltpu.CompilerParams(vmem_limit_bytes=56 * 1024 * 1024),
        cost_estimate=pl.CostEstimate(
            flops=20 * length * width * BLOCK, bytes_accessed=8 * length * width, transcendentals=0
        ),
        name="mixer",
    )(x, rows, taps, step, decay, step.T, decay.T)


def project_kernel(
    first_ref, second_ref, gate_ref, norm_gain_ref, matrix_ref, resid_ref, out_gain_ref, ffn_gain_ref,
    resid_one_ref, ffn_in_ref, normed, projected,
):
    step = pl.program_id(0)
    chunks, tok_rows, width = first_ref.shape
    per_group = chunks // GROUPS

    @pl.when(step == 0)
    def _():
        for group in range(GROUPS):
            total = jnp.zeros((tok_rows, 1), jnp.float32)
            for i in range(2 * group * per_group, 2 * (group + 1) * per_group):
                cols = slice(i * width, (i + 1) * width)
                heads_ref = (first_ref, second_ref)[i % 2]
                u = heads_ref[i // 2].astype(jnp.float32) * silu(gate_ref[:, cols].astype(jnp.float32))
                total = total + jnp.sum(u * u, axis=1, keepdims=True)
            scale = lax.rsqrt(total * (1.0 / (2 * per_group * width)) + EPS)
            for i in range(2 * group * per_group, 2 * (group + 1) * per_group):
                cols = slice(i * width, (i + 1) * width)
                heads_ref = (first_ref, second_ref)[i % 2]
                u = heads_ref[i // 2].astype(jnp.float32) * silu(gate_ref[:, cols].astype(jnp.float32))
                normed[:, cols] = (u * scale * norm_gain_ref[:, cols]).astype(jnp.bfloat16)

    parts, _, part = projected.shape
    projected[step] = jnp.dot(normed[...], matrix_ref[0], preferred_element_type=jnp.float32)

    @pl.when(step == pl.num_programs(0) - 1)
    def _():
        total = jnp.zeros((tok_rows, 1), jnp.float32)
        for j in range(parts):
            total = total + jnp.sum(projected[j] * projected[j], axis=1, keepdims=True)
        scale = lax.rsqrt(total * (1.0 / (parts * part)) + EPS)
        total = jnp.zeros((tok_rows, 1), jnp.float32)
        for j in range(parts):
            cols = slice(j * part, (j + 1) * part)
            one = (
                resid_ref[:, cols].astype(jnp.float32) + projected[j] * scale * out_gain_ref[:, cols]
            ).astype(jnp.bfloat16)
            resid_one_ref[:, cols] = one
            one = one.astype(jnp.float32)
            total = total + jnp.sum(one * one, axis=1, keepdims=True)
        scale = lax.rsqrt(total * (1.0 / (parts * part)) + EPS)
        for j in range(parts):
            cols = slice(j * part, (j + 1) * part)
            ffn_in_ref[:, cols] = (
                resid_one_ref[:, cols].astype(jnp.float32) * scale * ffn_gain_ref[:, cols]
            ).astype(jnp.bfloat16)


def run_project(heads, others, gate, norm_gain, matrix, resid, out_gain, ffn_gain):
    _, tok_rows, _ = heads.shape
    parts, inner, part = matrix.shape
    model = parts * part

    def whole(shape):
        return pl.BlockSpec(shape, lambda j: (0,) * len(shape))

    return pl.pallas_call(
        project_kernel,
        grid=(parts,),
        out_shape=(
            jax.ShapeDtypeStruct((tok_rows, model), jnp.bfloat16),
            jax.ShapeDtypeStruct((tok_rows, model), jnp.bfloat16),
        ),
        in_specs=[
            whole(heads.shape),
            whole(others.shape),
            whole(gate.shape),
            whole((1, inner)),
            pl.BlockSpec((1, inner, part), lambda j: (j, 0, 0)),
            whole(resid.shape),
            whole((1, model)),
            whole((1, model)),
        ],
        out_specs=(whole((tok_rows, model)), whole((tok_rows, model))),
        scratch_shapes=[
            pltpu.VMEM((tok_rows, inner), jnp.bfloat16),
            pltpu.VMEM((parts, tok_rows, part), jnp.float32),
        ],
        compiler_params=pltpu.CompilerParams(vmem_limit_bytes=50 * 1024 * 1024),
        cost_estimate=pl.CostEstimate(
            flops=2 * tok_rows * inner * model, bytes_accessed=2 * inner * model, transcendentals=0
        ),
        name="project",
    )(heads, others, gate, norm_gain[None], matrix, resid, out_gain[None], ffn_gain[None])


def local(
    resid,
    mixer_inputs,
    output_gate,
    write_rows_input,
    read_rows_input,
    step_size_logits,
    extra_log_decay,
    mixer_conv_taps,
    write_conv_taps,
    read_conv_taps,
    step_size_bias,
    decay_speed,
    grouped_norm_gain,
    output_matrix,
    output_gain,
    feedforward_gain,
    routes,
    route_weights,
    expert_gate_weight,
    expert_up_weight,
    expert_down_weight,
    expert_sum_gain,
):
    tok_rows = mixer_inputs.shape[1]
    local_heads = step_size_bias.shape[0]
    per_group = HEADS // GROUPS
    width = local_heads * HEAD_DIM
    sp_size = lax.axis_size("sp")
    my_sp = lax.axis_index("sp")
    group_id = my_sp * local_heads // per_group
    matrix = lax.all_gather(output_matrix, "dp", axis=0, tiled=False)

    def by_group(item):
        grouped = jnp.moveaxis(item.reshape(tok_rows, GROUPS, STATE), 1, 0)
        return jnp.repeat(grouped, sp_size // GROUPS, axis=0)

    part_heads = local_heads // 2
    part_width = part_heads * HEAD_DIM
    dirs = 2 * part_heads
    col_start = group_id * STATE
    row_taps = [
        lax.dynamic_slice_in_dim(item, col_start, STATE, 1) for item in (write_conv_taps, read_conv_taps)
    ]

    def to_send(part, rows):
        heads = slice(part * part_heads, (part + 1) * part_heads)
        small = [
            jnp.moveaxis(
                item[0].reshape(tok_rows, sp_size, local_heads, 2)[:, :, heads], (1, 3), (0, 2)
            ).reshape(sp_size, tok_rows, dirs)
            for item in (step_size_logits, extra_log_decay)
        ]
        channels = mixer_inputs[0].reshape(tok_rows, sp_size, width)
        channels = channels[:, :, part * part_width : (part + 1) * part_width]
        return jnp.concatenate([jnp.moveaxis(channels, 1, 0), *rows, *small], axis=2)

    def mix(part, received, rows):
        heads = slice(part * part_heads, (part + 1) * part_heads)
        small = received[:, received.shape[1] - 2 * dirs :].astype(jnp.float32)
        step = jax.nn.softplus(small[:, :dirs] + step_size_bias[heads].T.reshape(1, dirs))
        decay = small[:, dirs:] - decay_speed[heads].T.reshape(1, dirs) * step
        part_taps = mixer_conv_taps[:, part * part_width : (part + 1) * part_width]
        taps = jnp.concatenate([part_taps, *row_taps], axis=1).astype(jnp.float32)
        mixed = run_mixer(part_heads, received, rows, taps, step, decay)
        return mixed.reshape(sp_size, tok_rows, part_width)

    def exchange(item):
        return lax.all_to_all(item, "sp", split_axis=0, concat_axis=0, tiled=True)

    sent_first = to_send(0, [by_group(write_rows_input[0]), by_group(read_rows_input[0])])
    sent_second = to_send(1, [])
    first = exchange(sent_first)
    first, sent_second = lax.optimization_barrier((first, sent_second))
    second = exchange(sent_second).reshape(sp_size * tok_rows, -1)
    first = first.reshape(sp_size * tok_rows, -1)
    mixed_first = mix(0, first, first)
    second, mixed_first = lax.optimization_barrier((second, mixed_first))
    heads_first = exchange(mixed_first)
    mixed_second = mix(1, second, first)
    heads_second = exchange(mixed_second)
    resid_one, ffn_in = run_project(
        heads_first, heads_second, output_gate[0], grouped_norm_gain, matrix, resid[0], output_gain, feedforward_gain
    )
    local_experts = expert_gate_weight.shape[0]
    experts = local_experts * sp_size
    capacity = 3 * tok_rows * TOPK // (2 * experts)
    my_routes = routes[0]
    one_hot = (my_routes[:, :, None] == jnp.arange(experts, dtype=jnp.int32)).astype(jnp.int32)
    per_token = jnp.sum(one_hot, axis=1)
    earlier = jnp.cumsum(per_token, axis=0) - per_token
    slot_dest = my_routes * capacity + jnp.sum(earlier[:, None, :] * one_hot, axis=2)
    named = per_token.T
    place = jnp.where(named > 0, earlier.T, -1)
    slots = jnp.arange(capacity, dtype=jnp.int32)
    tokens = jnp.arange(tok_rows, dtype=jnp.int32)
    slot_token = jnp.sum(
        jnp.where(place[:, None, :] == slots[None, :, None], tokens, 0), axis=2
    )
    send_rows = ffn_in[slot_token.reshape(-1)].reshape(sp_size, local_experts, capacity, D)
    arrived = lax.all_to_all(send_rows, "sp", split_axis=0, concat_axis=0, tiled=True)
    gate_part = jnp.einsum(
        "sekd,edh->sekh", arrived, expert_gate_weight, preferred_element_type=jnp.float32
    )
    up_part = jnp.einsum(
        "sekd,edh->sekh", arrived, expert_up_weight, preferred_element_type=jnp.float32
    )
    hidden = (jax.nn.silu(gate_part) * up_part).astype(jnp.bfloat16)
    expert_rows = jnp.einsum(
        "sekh,ehd->sekd", hidden, expert_down_weight, preferred_element_type=jnp.float32
    ).astype(jnp.bfloat16)
    returned = lax.all_to_all(expert_rows, "sp", split_axis=0, concat_axis=0, tiled=True)
    returned = returned.reshape(experts * capacity, D)
    combined = sum(
        returned[slot_dest[:, k]].astype(jnp.float32) * route_weights[0][:, k : k + 1]
        for k in range(TOPK)
    )
    mixed_out = resid_one.astype(jnp.float32) + rms_scale(combined, expert_sum_gain)
    return mixed_out.astype(jnp.bfloat16)[None]


def solution(mesh):
    in_specs = (
        P("dp", "sp", None),
        P("dp", "sp", None),
        P("dp", "sp", None),
        P("dp", "sp", None),
        P("dp", "sp", None),
        P("dp", "sp", None, None),
        P("dp", "sp", None, None),
        P(None, "sp"),
        P(),
        P(),
        P("sp", None),
        P("sp", None),
        P(),
        P(None, "dp"),
        P(),
        P(),
        P("dp", "sp", None),
        P("dp", "sp", None),
        P("sp", None, None),
        P("sp", None, None),
        P("sp", None, None),
        P(),
    )
    out_specs = P("dp", "sp", None)
    return jax.shard_map(local, mesh=mesh, in_specs=in_specs, out_specs=out_specs, check_vma=False)
```
